32 devices in a mesh: sp: 8 (over z, x), tp: 4 (over y, core).
Axes of the slice: x: 2, y: 2, z: 4, core: 2. Of those that a mesh axis runs over, the one named last changes fastest.
Arguments:
- out_cotangent: bfloat16 [2048, 2048], P('sp'), may hold values from -6 to 6
- stream: bfloat16 [2048, 2048], P('sp'), may hold values from -6 to 6
- route_ids: int32 [2048, 2], P('sp'), may hold values from 0 to 7, all different within a row; in each aligned block of 256 rows (0 to 255, 256 to 511, ...) at most 128 rows name the same one
- route_weights: float32 [2048, 2], P('sp'), may hold values from 0.3 to 2
- gate_proj: bfloat16 [8, 2048, 1024], P('sp', None, 'tp'), may hold values from -0.125 to 0.125
- up_proj: bfloat16 [8, 2048, 1024], P('sp', None, 'tp'), may hold values from -0.125 to 0.125
- down_proj: bfloat16 [8, 1024, 2048], P('sp', 'tp'), may hold values from -0.1875 to 0.1875
- outer_gate: bfloat16 [2048, 512], P('sp', 'tp'), may hold values from -6 to 6
- inner_gate: bfloat16 [2048, 512], P('sp', 'tp'), may hold values from -6 to 6
- conv_input: bfloat16 [2048, 512], P('sp', 'tp'), may hold values from -6 to 6
- conv_taps: float32 [3, 512], P(None, 'tp'), may hold values from -4 to 4
- out_proj: bfloat16 [2048, 512], P(None, 'tp'), may hold values from -0.25 to 0.25
Outputs:
- grad_gate_proj: bfloat16 [8, 2048, 1024], P('sp', None, 'tp')
- grad_up_proj: bfloat16 [8, 2048, 1024], P('sp', None, 'tp')
- grad_down_proj: bfloat16 [8, 1024, 2048], P('sp', 'tp')
- grad_out_proj: float32 [2048, 512], P('sp', 'tp')
- grad_outer_gate: float32 [2048, 512], P('sp', 'tp')
- grad_inner_gate: float32 [2048, 512], P('sp', 'tp')
- grad_conv_input: float32 [2048, 512], P('sp', 'tp')
The draws below stay inside these ranges and needn't reach their ends.
Inputs may be any that keep to these rules, and one draw needn't show every extreme that they name: `route_ids`: the 2 experts of a token differ. Among the tokens of one index of sp, no expert is chosen more than 128 times, and in every draw some expert is chosen exactly 128 times by them.
All inputs are finite; a program needn't handle non-finite values.
Results may differ from the reference program's by a relative error of at most 0.018.
Values may be sent and summed in bfloat16 or wider, within the bound.
No kernel may reach another device: no remote copies, remote signals or barrier semaphores. Data moves between devices by JAX's collectives and lax.ppermute only.
A program may use at most 64 MiB of HBM per device.

```python
import math
import jax
import jax.numpy as jnp
import numpy as np
from jax import lax

D = 2048
FF = 1024
CONV = 512
TAPS = 3
TOPK = 2
TOK_DEV = 256
EXPERTS = 8
CAP = 128
SLOTS = 1024
TOKENS = 2048
N_TP = 4


def with_spikes(entries, rng, source, target, shards_of, factor):
    owner, partner = [(jnp.arange(entries.shape[dim]) // (entries.shape[dim] // shards_of)).reshape([-1 if axis == dim else 1 for axis in range(entries.ndim)]) for dim in (source, target)]
    chosen = jax.random.permutation(rng, shards_of)[partner]
    strong = (owner == chosen) | (owner == (partner + shards_of // 2) % shards_of)
    return jnp.where(strong, factor * entries, entries)


def block_levels(stream_key, dims, cuts, low, largest):
    def one(dim, parts):
        heights = jax.random.uniform(jax.random.fold_in(jax.random.fold_in(stream_key, 6), dim), (parts,), jnp.float32, low / len(cuts), largest / len(cuts))
        return jnp.repeat(jnp.exp(heights), dims[dim] // parts).reshape((-1,) + (1,) * (len(dims) - dim - 1))

    gain = one(*cuts[0])
    for cut in cuts[1:]:
        gain = gain * one(*cut)
    return gain


def deal_out(own_key, own, number, rows, count, top, reach, lean):
    sequence = jax.random.permutation(own_key, count)
    heavy_load, ordinary = shares(count, rows * top, reach, lean, True), shares(count, rows * top, reach, lean, False)
    places = jnp.arange(count)

    def named(tallies, turn):
        used = int((tallies > 0).sum())
        fixed = max(1, used // 4)
        moved = fixed + (places - fixed + turn * (used - fixed)) % max(1, count - fixed)
        return jnp.zeros((count,), jnp.int32).at[sequence[jnp.where(places < fixed, places, moved)]].set(jnp.asarray(tallies, jnp.int32))

    tallies = jnp.where(number % 4 == 0, named(heavy_load, number // 4), named(ordinary, number - number // 4 - 1))
    mixed = jax.random.permutation(jax.random.fold_in(own, 3), count)
    donor, sink = mixed[0:count // 2 * 2:2], mixed[1:count // 2 * 2:2]
    room = jnp.minimum(tallies[donor] - 1, reach - tallies[sink]) // 2
    room = jnp.where((donor == sequence[0]) | (sink == sequence[0]) | (tallies[sink] == 0), 0, jnp.maximum(room, 0))
    moved = jax.random.randint(jax.random.fold_in(own, 4), (count // 2,), 0, 1 << 20) % (room + 1)
    tallies = tallies.at[donor].add(-moved).at[sink].add(moved)
    labels = jnp.searchsorted(jnp.cumsum(tallies), jnp.arange(rows * top), side="right").astype(jnp.int32)
    table = labels.reshape(top, rows).T
    table = table[jax.random.permutation(jax.random.fold_in(own, 1), rows)]
    turn = jax.random.randint(jax.random.fold_in(own, 2), (rows, 1), 0, top)
    return jnp.take_along_axis(table, (jnp.arange(top)[None, :] + turn) % top, axis=1)


def shares(number_of, total, reach, skew, full):
    portions = [(1 << 20) // math.isqrt(grade ** skew) + 1 for grade in range(1, number_of + 1)]
    largest = reach if full else min(reach, max(-(-total // number_of), total * portions[0] // sum(portions)))
    least = 1 if total - largest >= number_of - 1 else 0
    counts, rest = [largest] + [least] * (number_of - 1), total - largest - least * (number_of - 1)
    while rest > 0:
        movable = [i for i in range(1, number_of) if counts[i] < largest] or [i for i in range(1, number_of) if counts[i] < reach]
        whole, left = sum([portions[i] for i in movable]), rest
        for i in movable:
            more = min(reach - counts[i], max(1, left * portions[i] // whole), rest)
            counts[i] = counts[i] + more
            rest = rest - more
    return np.array(counts)


def bell_draw(own_key, dims, deviation, bound, cuts=(), kind=jnp.bfloat16):
    loudness = block_levels(own_key, dims, cuts, -0.22, 0.18) if cuts else 1.0
    entries = jax.random.normal(own_key, dims, jnp.float32) * deviation * loudness
    return jnp.minimum(jnp.maximum(entries, -bound), bound).astype(kind)


def bell_draw_with(stream_key, extent, width, most, cuts, heavy, kind=jnp.bfloat16):
    values = width * jax.random.normal(stream_key, extent, jnp.float32)
    if cuts:
        values = values * block_levels(stream_key, extent, cuts, -0.22, 0.18)
    return jnp.clip(with_spikes(values, jax.random.fold_in(stream_key, 3), *heavy), -most, most).astype(kind)


def setup_inputs(seed: int = 0) -> dict:
    seeds = jax.random.split(jax.random.key(seed), 13)
    out_cotangent = bell_draw_with(seeds[0], (TOKENS, D), 1.0, 6.0, ((0, 8),), (0, 1, 8, 2.0))
    stream = bell_draw(seeds[1], (TOKENS, D), 1.0, 6.0, ((0, 8),))
    route_ids_keys = jax.random.split(jax.random.fold_in(seeds[2], 1), TOKENS // TOK_DEV)
    route_ids_turns = jax.random.permutation(jax.random.fold_in(seeds[2], 3), TOKENS // TOK_DEV)
    route_ids = jax.vmap(lambda own, number: deal_out(jax.random.fold_in(seeds[2], 2), own, number, TOK_DEV, EXPERTS, TOPK, CAP, 1))(route_ids_keys, route_ids_turns).reshape((TOKENS, TOPK))
    route_weights = jnp.clip(0.3 + 1.7 * jax.random.uniform(seeds[3], (TOKENS, TOPK), jnp.float32) ** block_levels(seeds[3], (TOKENS, TOPK), ((0, 8),), -0.2, 0.2), 0.3, 2.0)
    gate_proj = bell_draw(seeds[4], (EXPERTS, D, FF), D ** -0.5, 0.125, ((0, 8), (2, 4)))
    up_proj = bell_draw(seeds[5], (EXPERTS, D, FF), D ** -0.5, 0.125, ((0, 8), (2, 4)))
    down_proj = bell_draw(seeds[6], (EXPERTS, FF, D), FF ** -0.5, 0.1875, ((0, 8), (1, 4)))
    outer_gate = bell_draw(seeds[7], (TOKENS, CONV), 1.0, 6.0, ((0, 8), (1, 4)))
    inner_gate = bell_draw(seeds[8], (TOKENS, CONV), 1.0, 6.0, ((0, 8), (1, 4)))
    conv_input = bell_draw(seeds[9], (TOKENS, CONV), 1.0, 6.0, ((0, 8), (1, 4)))
    conv_taps = bell_draw(seeds[10], (TAPS, CONV), 0.6, 4.0, ((1, 4),), jnp.float32)
    out_proj = bell_draw(seeds[11], (D, CONV), CONV ** -0.5, 0.25, ((1, 4),))
    return dict(out_cotangent=out_cotangent, stream=stream, route_ids=route_ids, route_weights=route_weights, gate_proj=gate_proj, up_proj=up_proj, down_proj=down_proj, outer_gate=outer_gate, inner_gate=inner_gate, conv_input=conv_input, conv_taps=conv_taps, out_proj=out_proj)


def expert_backward(out_cotangent, stream, route_ids, route_weights, w_gate, w_up, w_down, expert):
    chosen = route_ids == expert
    weight = jnp.sum(jnp.where(chosen, route_weights, 0.0), axis=1)
    hit = jnp.any(chosen, axis=1)
    index = jnp.nonzero(hit, size=SLOTS, fill_value=0)[0].astype(jnp.int32)
    count = jnp.sum(hit.astype(jnp.int32))
    valid = jnp.arange(SLOTS, dtype=jnp.int32) < count
    rows_input = jnp.where(valid[:, None], stream[index], jnp.zeros((), jnp.bfloat16))
    rows_grad = (weight[index][:, None] * out_cotangent[index].astype(jnp.float32))
    rows_grad = jnp.where(valid[:, None], rows_grad, 0.0).astype(jnp.bfloat16)
    gate = jnp.dot(rows_input, w_gate, preferred_element_type=jnp.float32)
    up = jnp.dot(rows_input, w_up, preferred_element_type=jnp.float32)
    sig = jax.nn.sigmoid(gate)
    silu_gate = gate * sig
    hidden = (silu_gate * up).astype(jnp.bfloat16)
    d_hidden = lax.dot_general(rows_grad, w_down, (((1,), (1,)), ((), ())), preferred_element_type=jnp.float32)
    d_gate = (d_hidden * up * sig * (1.0 + gate * (1.0 - sig))).astype(jnp.bfloat16)
    d_up = (d_hidden * silu_gate).astype(jnp.bfloat16)
    over_rows = (((0,), (0,)), ((), ()))
    grad_down = lax.dot_general(hidden, rows_grad, over_rows, preferred_element_type=jnp.float32).astype(jnp.bfloat16)
    grad_gate = lax.dot_general(rows_input, d_gate, over_rows, preferred_element_type=jnp.float32).astype(jnp.bfloat16)
    grad_up = lax.dot_general(rows_input, d_up, over_rows, preferred_element_type=jnp.float32).astype(jnp.bfloat16)
    block = FF // N_TP
    gate_blocks = d_gate.astype(jnp.float32).reshape(SLOTS, N_TP, block)
    up_blocks = d_up.astype(jnp.float32).reshape(SLOTS, N_TP, block)
    wg_blocks = w_gate.astype(jnp.float32).reshape(D, N_TP, block)
    wu_blocks = w_up.astype(jnp.float32).reshape(D, N_TP, block)
    partials = jnp.einsum('snf,dnf->nsd', gate_blocks, wg_blocks) + jnp.einsum('snf,dnf->nsd', up_blocks, wu_blocks)
    partials = partials.astype(jnp.bfloat16).astype(jnp.float32)
    row_grad = jnp.sum(partials, axis=0).astype(jnp.bfloat16)
    row_grad = jnp.where(valid[:, None], row_grad.astype(jnp.float32), 0.0)
    return index, row_grad, grad_gate, grad_up, grad_down


def reference(out_cotangent, stream, route_ids, route_weights, gate_proj, up_proj, down_proj,
              outer_gate, inner_gate, conv_input, conv_taps, out_proj):
    def step(carry, inputs):
        w_gate, w_up, w_down, expert = inputs
        index, row_grad, grad_gate, grad_up, grad_down = expert_backward(
            out_cotangent, stream, route_ids, route_weights, w_gate, w_up, w_down, expert)
        carry = carry.at[index].add(row_grad)
        return carry, (grad_gate, grad_up, grad_down)

    moe_grad, grads = lax.scan(step, jnp.zeros((TOKENS, D), jnp.float32),
                               (gate_proj, up_proj, down_proj, jnp.arange(EXPERTS, dtype=jnp.int32)))
    grad_gate_proj, grad_up_proj, grad_down_proj = grads
    stream_grad = (out_cotangent.astype(jnp.float32) + moe_grad).astype(jnp.bfloat16)
    mixed = inner_gate.astype(jnp.float32) * conv_input.astype(jnp.float32)
    padded = jnp.concatenate([jnp.zeros((2, CONV), jnp.float32), mixed], axis=0)
    conv_out = conv_taps[0] * padded[:TOKENS] + conv_taps[1] * padded[1:TOKENS + 1] + conv_taps[2] * padded[2:]
    mixer_out = (outer_gate.astype(jnp.float32) * conv_out).astype(jnp.bfloat16)
    d_mixer = jnp.dot(stream_grad, out_proj, preferred_element_type=jnp.float32)
    grad_outer_gate = d_mixer * conv_out
    d_conv = d_mixer * outer_gate.astype(jnp.float32)
    trailing = jnp.concatenate([d_conv, jnp.zeros((2, CONV), jnp.float32)], axis=0)
    d_mixed = conv_taps[2] * trailing[:TOKENS] + conv_taps[1] * trailing[1:TOKENS + 1] + conv_taps[0] * trailing[2:]
    grad_inner_gate = d_mixed * conv_input.astype(jnp.float32)
    grad_conv_input = d_mixed * inner_gate.astype(jnp.float32)
    grad_out_proj = lax.dot_general(stream_grad, mixer_out, (((0,), (0,)), ((), ())), preferred_element_type=jnp.float32)
    return (grad_gate_proj, grad_up_proj, grad_down_proj, grad_out_proj,
            grad_outer_gate, grad_inner_gate, grad_conv_input)
```

```python
import functools

import jax
import jax.numpy as jnp
from jax import lax
from jax.experimental import pallas as pl
from jax.experimental.pallas import tpu as pltpu
from jax.sharding import PartitionSpec as P


MOST_PERMUTES = 16
ACROSS = (((1,), (1,)), ((), ()))
OVER_ROWS = (((0,), (0,)), ((), ()))
F32 = jnp.float32
BF16 = jnp.bfloat16


def partner(x, axis, by, scope):
    n = lax.axis_size(axis)
    with jax.named_scope(scope):
        return lax.ppermute(x, axis, [(i, i ^ by) for i in range(n)])


def passed_along(x, axis, by):
    devices = lax.axis_size(axis)
    pairs = [(i, i + by) for i in range(devices) if 0 <= i + by < devices]
    return lax.ppermute(x, axis, pairs)


def halving_order(n):
    order = [0]
    by = n // 2
    while by >= 1:
        order = order + [j ^ by for j in order] if by == n // 2 else [
            j for j in order
        ] + [j ^ by for j in order]
        by //= 2
    return order


def gathered(x, axis, scope):
    n = lax.axis_size(axis)
    parts = {0: x}
    by = n // 2
    while by >= 1:
        for j in list(parts):
            parts[j ^ by] = partner(parts[j], axis, by, f"{scope}_{j ^ by}")
        by //= 2
    return [parts[j] for j in range(n)]


def halved_sum(keep, send, axis, scope):
    n = lax.axis_size(axis)
    by = 1
    while by < n:
        got = partner(send, axis, by, f"{scope}_{by}")
        total = keep.astype(F32) + got.astype(F32)
        by *= 2
        if by < n:
            half = total.shape[1] // 2
            keep, send = total[:, :half], total[:, half:].astype(BF16)
    return total


def rows_kernel(nt, nb, q_ref, *refs):
    blocks = [refs[b * nt : (b + 1) * nt] for b in range(nb)]
    wg, wu, wd, mix = refs[nb * nt : nb * nt + 4]
    dgu, hid, keep, send, outer = refs[nb * nt + 4 :]
    q = q_ref[0]
    rows = blocks[0][0].shape[0]
    width = wg.shape[0]
    part = width // nt
    hidden_units = wg.shape[1]
    order = halving_order(nt)
    chan = blocks[0][0].shape[1] - 2 * part
    step = 256 if (nb * rows) % 256 == 0 else rows
    for start in range(0, nb * rows, step):
        pieces = []
        at = start
        while at < start + step:
            b, r = divmod(at, rows)
            size = min(rows - r, start + step - at)
            pieces.append((b, r, size))
            at += size

        def cols(j, lo, hi):
            got = [blocks[b][j][r : r + s, lo:hi] for b, r, s in pieces]
            return got[0] if len(got) == 1 else jnp.concatenate(got, axis=0)

        gate = up = d_hidden = None
        for j in range(nt):
            at_w = pl.ds(pl.multiple_of((q ^ j) * part, part), part)
            xj = cols(j, 0, part)
            gj = cols(j, part, 2 * part)
            a = jnp.dot(xj, wg[at_w, :], preferred_element_type=F32)
            u = jnp.dot(xj, wu[at_w, :], preferred_element_type=F32)
            d = lax.dot_general(gj, wd[:, at_w], ACROSS, preferred_element_type=F32)
            gate = a if gate is None else gate + a
            up = u if up is None else up + u
            d_hidden = d if d_hidden is None else d_hidden + d
        sig = jax.nn.sigmoid(gate)
        silu = gate * sig
        d_gate = (d_hidden * up * sig * (1.0 + gate * (1.0 - sig))).astype(BF16)
        d_up = (d_hidden * silu).astype(BF16)
        here = pl.ds(start, step)
        hid[here, :] = (silu * up).astype(BF16)
        dgu[here, :hidden_units] = d_gate
        dgu[here, hidden_units:] = d_up
        both = jnp.concatenate([d_gate, d_up], axis=1)
        r = jnp.dot(both, mix[...], preferred_element_type=F32).astype(BF16)
        half = r.shape[1] // 2
        keep[here, :] = r[:, :half]
        send[here, :] = r[:, half:]
        m_rows = jnp.concatenate([cols(j, 2 * part, 2 * part + chan) for j in order], axis=1)
        o = lax.dot_general(both, m_rows, OVER_ROWS, preferred_element_type=F32)
        if start == 0:
            outer[...] = o
        else:
            outer[...] += o


def expert_rows(q, blocks, wg, wu, wd, mix):
    nb, nt = len(blocks), len(blocks[0])
    rows = nb * blocks[0][0].shape[0]
    ff = wg.shape[1]
    chans = mix.shape[1]
    vmem = pl.BlockSpec(memory_space=pltpu.VMEM)
    flops = 2 * rows * ff * (3 * wg.shape[0] + 4 * chans)
    return pl.pallas_call(
        functools.partial(rows_kernel, nt, nb),
        out_shape=(
            jax.ShapeDtypeStruct((rows, 2 * ff), BF16),
            jax.ShapeDtypeStruct((rows, ff), BF16),
            jax.ShapeDtypeStruct((rows, chans // 2), BF16),
            jax.ShapeDtypeStruct((rows, chans // 2), BF16),
            jax.ShapeDtypeStruct((2 * ff, chans), F32),
        ),
        in_specs=[pl.BlockSpec(memory_space=pltpu.SMEM)] + [vmem] * (nb * nt + 4),
        out_specs=(vmem,) * 5,
        cost_estimate=pl.CostEstimate(flops=flops, bytes_accessed=8 << 20, transcendentals=rows * ff),
    )(q, *[x for b in blocks for x in b], wg, wu, wd, mix)


def grads_kernel(nt, nb, ng, q_ref, *refs):
    blocks = [refs[b * nt : (b + 1) * nt] for b in range(nb)]
    dgus = refs[nb * nt : nb * nt + ng]
    hids = refs[nb * nt + ng : nb * nt + 2 * ng]
    g_gate, g_up, g_down = refs[nb * nt + 2 * ng :]
    q = q_ref[0]
    rows = blocks[0][0].shape[0]
    width, ff = g_gate.shape
    part = width // nt
    per = dgus[0].shape[0]
    step = 256 if (nb * rows) % 256 == 0 and per % 256 == 0 else rows
    tile = min(256, part)

    def cols(j, start, lo, hi):
        got = []
        at = start
        while at < start + step:
            b, r = divmod(at, rows)
            size = min(rows - r, start + step - at)
            got.append(blocks[b][j][r : r + size, lo:hi])
            at += size
        return got[0] if len(got) == 1 else jnp.concatenate(got, axis=0)

    for j in range(nt):
        for lo in range(0, part, tile):
            acc = down = None
            for start in range(0, nb * rows, step):
                g, r = divmod(start, per)
                xj = cols(j, start, lo, lo + tile)
                gj = cols(j, start, part + lo, part + lo + tile)
                a = lax.dot_general(xj, dgus[g][r : r + step, :], OVER_ROWS, preferred_element_type=F32)
                d = lax.dot_general(hids[g][r : r + step, :], gj, OVER_ROWS, preferred_element_type=F32)
                acc = a if acc is None else acc + a
                down = d if down is None else down + d
            at_w = pl.ds(pl.multiple_of((q ^ j) * part + lo, tile), tile)
            g_gate[at_w, :] = acc[:, :ff].astype(BF16)
            g_up[at_w, :] = acc[:, ff:].astype(BF16)
            g_down[:, at_w] = down.astype(BF16)


def expert_grads(q, blocks, dgus, hids, width):
    nb, nt, ng = len(blocks), len(blocks[0]), len(dgus)
    ff = hids[0].shape[1]
    rows = nb * blocks[0][0].shape[0]
    vmem = pl.BlockSpec(memory_space=pltpu.VMEM)
    return pl.pallas_call(
        functools.partial(grads_kernel, nt, nb, ng),
        out_shape=(
            jax.ShapeDtypeStruct((width, ff), BF16),
            jax.ShapeDtypeStruct((width, ff), BF16),
            jax.ShapeDtypeStruct((ff, width), BF16),
        ),
        in_specs=[pl.BlockSpec(memory_space=pltpu.SMEM)] + [vmem] * (nb * nt + 2 * ng),
        out_specs=(vmem,) * 3,
        cost_estimate=pl.CostEstimate(
            flops=6 * rows * ff * width, bytes_accessed=16 << 20, transcendentals=0
        ),
    )(q, *[x for b in blocks for x in b], *dgus, *hids)


def shards(
    out_cotangent,
    stream,
    route_ids,
    route_weights,
    gate_proj,
    up_proj,
    down_proj,
    outer_gate,
    inner_gate,
    conv_input,
    conv_taps,
    out_proj,
):
    ns = lax.axis_size("sp")
    nt = lax.axis_size("tp")
    me = lax.axis_index("sp")
    q = lax.axis_index("tp")
    tokens_here, width = stream.shape
    part = width // nt
    experts = ns * gate_proj.shape[0]
    capacity = 4 * tokens_here // experts
    q_arr = q.astype(jnp.int32).reshape(1)
    order = halving_order(nt)
    swaps = ns <= MOST_PERMUTES

    mixed = inner_gate.astype(F32) * conv_input.astype(F32)
    previous = passed_along(mixed[tokens_here - 2 :], "sp", 1)
    proj_parts = gathered(out_proj, "tp", "proj")
    extended = jnp.concatenate([previous, mixed], axis=0)
    conv_out = (
        conv_taps[0] * extended[:tokens_here]
        + conv_taps[1] * extended[1 : tokens_here + 1]
        + conv_taps[2] * extended[2:]
    )
    mixer_out = (outer_gate.astype(F32) * conv_out).astype(BF16)

    steps = jnp.arange(ns, dtype=jnp.int32)
    peer = me ^ steps if swaps else steps
    names = route_ids[None, :, :] == peer[:, None, None]
    hit = jnp.any(names, axis=2)
    weight = jnp.sum(jnp.where(names, route_weights[None], 0.0), axis=2)
    tok = jnp.arange(tokens_here, dtype=jnp.int32)
    before = (tok[:, None] < tok[None, :]).astype(BF16)
    rank = jnp.dot(hit.astype(BF16), before, preferred_element_type=F32).astype(jnp.int32)
    slot = jnp.where(hit, rank, -1)
    taken = slot[:, None, :] == jnp.arange(capacity, dtype=jnp.int32)[None, :, None]
    pick = taken.astype(BF16).reshape(ns * capacity, tokens_here)
    slot_weight = jnp.sum(jnp.where(taken, weight[:, None, :], 0.0), axis=2).reshape(-1, 1)
    own_x = lax.dynamic_slice_in_dim(stream, q * part, part, 1)
    own_g = lax.dynamic_slice_in_dim(out_cotangent, q * part, part, 1)
    sent = jnp.concatenate(
        [
            jnp.dot(pick, own_x, preferred_element_type=F32).astype(BF16),
            (slot_weight * jnp.dot(pick, own_g, preferred_element_type=F32)).astype(BF16),
            jnp.dot(pick, mixer_out, preferred_element_type=F32).astype(BF16),
        ],
        axis=1,
    )
    if swaps:
        sent = [sent[k * capacity : (k + 1) * capacity] for k in range(ns)]
        got = [partner(x, "sp", k, f"out_{k}") if k else x for k, x in enumerate(sent)]
    else:
        got = [
            lax.all_to_all(
                sent.reshape(ns, capacity, -1), "sp", split_axis=0, concat_axis=0, tiled=True
            ).reshape(ns * capacity, -1)
        ]
    blocks = [gathered(x, "tp", f"side_{k}") for k, x in enumerate(got)]

    w_gate, w_up, w_down = gate_proj[0], up_proj[0], down_proj[0]
    proj_all = jnp.concatenate([proj_parts[j] for j in order], axis=1)
    mix = jnp.concatenate(
        [
            lax.dot_general(w, proj_all, OVER_ROWS, preferred_element_type=F32).astype(BF16)
            for w in (w_gate, w_up)
        ],
        axis=0,
    )
    own_mixer = jnp.dot(out_cotangent, out_proj, preferred_element_type=F32)
    own_projection = lax.dot_general(
        out_cotangent, mixer_out, OVER_ROWS, preferred_element_type=F32
    )

    halves = [blocks[: len(blocks) // 2], blocks[len(blocks) // 2 :]] if swaps else [blocks]
    done = [expert_rows(q_arr, h, w_gate, w_up, w_down, mix) for h in halves]
    keep = jnp.concatenate([d[2] for d in done], axis=0)
    send = jnp.concatenate([d[3] for d in done], axis=0)
    share = halved_sum(keep, send, "tp", "back").astype(BF16)

    outer = sum(d[4] for d in done).astype(BF16)
    ff = w_gate.shape[1]
    spread = jnp.dot(w_gate, outer[:ff], preferred_element_type=F32) + jnp.dot(
        w_up, outer[ff:], preferred_element_type=F32
    )
    half = spread.shape[1] // 2
    proj_sum = halved_sum(spread[:, :half], spread[:, half:].astype(BF16), "tp", "grad")
    proj_sum = (proj_sum + own_projection).astype(BF16).reshape(ns, width // ns, -1)

    if swaps:
        back = jnp.concatenate(
            [
                partner(x, "sp", k, f"ret_{k}") if k else x
                for k, x in enumerate(jnp.split(share, ns, axis=0))
            ],
            axis=0,
        )
        turned = proj_sum[peer]
        shares = [
            partner(turned[k], "sp", k, f"fin_{k}") if k else turned[k] for k in range(ns)
        ]
        grad_projection = sum(s.astype(F32) for s in shares)
    else:
        back = lax.all_to_all(
            share.reshape(ns, capacity, -1), "sp", split_axis=0, concat_axis=0, tiled=True
        ).reshape(ns * capacity, -1)
        grad_projection = jnp.sum(
            lax.all_to_all(proj_sum, "sp", split_axis=0, concat_axis=0, tiled=True).astype(F32),
            axis=0,
        )

    d_mixer = own_mixer + lax.dot_general(pick, back, OVER_ROWS, preferred_element_type=F32)
    grad_outer = d_mixer * conv_out
    d_conv = d_mixer * outer_gate.astype(F32)
    following = passed_along(d_conv[:2], "sp", -1)
    trailing = jnp.concatenate([d_conv, following], axis=0)
    d_mixed = (
        conv_taps[2] * trailing[:tokens_here]
        + conv_taps[1] * trailing[1 : tokens_here + 1]
        + conv_taps[0] * trailing[2:]
    )
    grad_inner = d_mixed * conv_input.astype(F32)
    grad_input = d_mixed * inner_gate.astype(F32)

    grad_gate, grad_up, grad_down = expert_grads(
        q_arr, blocks, [d[0] for d in done], [d[1] for d in done], width
    )
    return (
        grad_gate[None],
        grad_up[None],
        grad_down[None],
        grad_projection,
        grad_outer,
        grad_inner,
        grad_input,
    )


def solution(mesh):
    placed = (
        P("sp", None),
        P("sp", None),
        P("sp", None),
        P("sp", None),
        P("sp", None, "tp"),
        P("sp", None, "tp"),
        P("sp", "tp", None),
        P("sp", "tp"),
        P("sp", "tp"),
        P("sp", "tp"),
        P(None, "tp"),
        P(None, "tp"),
    )
    return jax.shard_map(
        shards,
        mesh=mesh,
        in_specs=placed,
        out_specs=(
            P("sp", None, "tp"),
            P("sp", None, "tp"),
            P("sp", "tp", None),
            P("sp", "tp"),
            P("sp", "tp"),
            P("sp", "tp"),
            P("sp", "tp"),
        ),
        check_vma=False,
    )
```
